768 devices in a mesh: tp: 96 (over z, y), dp: 8 (over x, core).
Axes of the slice: x: 4, y: 8, z: 12, core: 2. Of those that a mesh axis runs over, the one named last changes fastest.
Arguments:
- tokens: bfloat16 [192, 8448], P('dp', 'tp'), may hold values from -6 to 6
- gains: float32 [2, 8448], replicated, may hold values from 0.1 to 1.9
- w_input: bfloat16 [2, 8448, 12288], P(None, 'dp', 'tp'), may hold values from -0.0625 to 0.0625
- w_gating: bfloat16 [2, 8448, 12288], P(None, 'dp', 'tp'), may hold values from -0.0625 to 0.0625
- w_output: bfloat16 [2, 12288, 8448], P(None, 'tp'), may hold values from -0.5 to 0.5
- decay_rate: float32 [2, 768, 64], P(None, 'tp'), may hold values from 0.05 to 2
- frequency: float32 [2, 768, 64], P(None, 'tp'), may hold values from -3 to 3
- log_step: float32 [2, 768], P(None, 'tp'), may hold values from -2.3 to 0
- in_real: float32 [2, 768, 64, 16], P(None, 'tp'), may hold values from -1 to 1
- in_imag: float32 [2, 768, 64, 16], P(None, 'tp'), may hold values from -1 to 1
- readout_real_matrix: float32 [2, 768, 16, 64], P(None, 'tp'), may hold values from -0.5 to 0.5
- readout_imag_matrix: float32 [2, 768, 16, 64], P(None, 'tp'), may hold values from -0.5 to 0.5
- skip_gain: float32 [2, 12288], P(None, 'tp'), may hold values from -4 to 4
- state_real: float32 [2, 192, 768, 64], P(None, 'dp', 'tp'), may hold values from -6 to 6
- state_imag: float32 [2, 192, 768, 64], P(None, 'dp', 'tp'), may hold values from -6 to 6
Outputs:
- mixed: bfloat16 [192, 8448], P('dp', 'tp')
- next_real: float32 [2, 192, 768, 64], P(None, 'dp', 'tp')
- next_imag: float32 [2, 192, 768, 64], P(None, 'dp', 'tp')
The draws below stay inside these ranges and needn't reach their ends.
All inputs are finite; a program needn't handle non-finite values.
Results may differ from the reference program's by a relative error of at most 0.008.
Values may be sent and summed in bfloat16 or wider, within the bound.
A program may use at most 64 MiB of HBM per device.

```python
import math
import jax
import jax.numpy as jnp
from jax import lax

D = 8448
G = 768
GS = 16
P_SIZE = 64
LAYERS = 2
BATCH = 192
W = 12288


def with_spikes(drawn, stream_key, source, target, shards_of, factor):
    owner, partner = [(jnp.arange(drawn.shape[position]) // (drawn.shape[position] // shards_of)).reshape([-1 if axis == position else 1 for axis in range(drawn.ndim)]) for position in (source, target)]
    chosen = jax.random.permutation(stream_key, shards_of)[partner]
    strong = (owner == chosen) | (owner == (partner + shards_of // 2) % shards_of)
    return jnp.where(strong, factor * drawn, drawn)


def steps_of(stream_key, shape, split, low, largest):
    def one(dim, shards_of):
        steps = jax.random.uniform(jax.random.fold_in(jax.random.fold_in(stream_key, 6), dim), (shards_of,), jnp.float32, low / len(split), largest / len(split))
        return jnp.repeat(jnp.exp(steps), shape[dim] // shards_of).reshape((-1,) + (1,) * (len(shape) - dim - 1))

    gain = one(*split[0])
    for cut in split[1:]:
        gain = gain * one(*cut)
    return gain


def gaussian(stream_key, shape, width, bound, pieces=(), dtype=jnp.bfloat16):
    entries = width * jax.random.normal(stream_key, shape, jnp.float32)
    if pieces:
        entries = entries * steps_of(stream_key, shape, pieces, -0.22, 0.18)
    return jnp.clip(entries, -bound, bound).astype(dtype)


def noise_with(rng, dims, width, bound, shards, heavy, kind=jnp.bfloat16):
    entries = width * jax.random.normal(rng, dims, jnp.float32)
    if shards:
        entries = entries * steps_of(rng, dims, shards, -0.22, 0.18)
    return jnp.clip(with_spikes(entries, jax.random.fold_in(rng, 3), *heavy), -bound, bound).astype(kind)


def setup_inputs(seed: int = 0) -> dict:
    streams_of = jax.random.split(jax.random.key(seed), 16)
    return {
        "tokens": gaussian(streams_of[0], (BATCH, D), 1.0, 6.0, ((0, 8), (1, 96))),
        "gains": jnp.clip(1.0 + 0.18 * jax.random.normal(streams_of[1], (LAYERS, D), jnp.float32), 0.1, 1.9),
        "w_input": gaussian(streams_of[2], (LAYERS, D, W), D ** -0.5, 0.0625, ((1, 8), (2, 96))),
        "w_gating": gaussian(streams_of[3], (LAYERS, D, W), D ** -0.5, 0.0625, ((1, 8), (2, 96))),
        "w_output": noise_with(streams_of[4], (LAYERS, W, D), (W // 8) ** -0.5, 0.5, ((1, 96),), (1, 2, 96, 4.75)),
        "decay_rate": jnp.clip(jnp.exp(math.log(2.0) - 3.6888794 * jax.random.uniform(streams_of[5], (LAYERS, G, P_SIZE), jnp.float32) ** steps_of(streams_of[5], (LAYERS, G, P_SIZE), ((1, 96),), -0.2, 0.2)), 0.05, 2.0),
        "frequency": jnp.clip(jax.random.uniform(streams_of[6], (LAYERS, G, P_SIZE), jnp.float32, -3.0, 3.0) * steps_of(streams_of[6], (LAYERS, G, P_SIZE), ((1, 96),), -0.4, 0.0), -3.0, 3.0),
        "log_step": jnp.clip(-2.3 + 2.3 * jax.random.uniform(streams_of[7], (LAYERS, G), jnp.float32) ** steps_of(streams_of[7], (LAYERS, G), ((1, 96),), -0.2, 0.2), -2.3, 0.0),
        "in_real": gaussian(streams_of[8], (LAYERS, G, P_SIZE, GS), (2 * GS) ** -0.5, 1.0, ((1, 96),), jnp.float32),
        "in_imag": gaussian(streams_of[9], (LAYERS, G, P_SIZE, GS), (2 * GS) ** -0.5, 1.0, ((1, 96),), jnp.float32),
        "readout_real_matrix": gaussian(streams_of[10], (LAYERS, G, GS, P_SIZE), (2 * P_SIZE) ** -0.5, 0.5, ((1, 96),), jnp.float32),
        "readout_imag_matrix": gaussian(streams_of[11], (LAYERS, G, GS, P_SIZE), (2 * P_SIZE) ** -0.5, 0.5, ((1, 96),), jnp.float32),
        "skip_gain": gaussian(streams_of[12], (LAYERS, W), 1.0, 4.0, ((1, 96),), jnp.float32),
        "state_real": gaussian(streams_of[13], (LAYERS, BATCH, G, P_SIZE), 1.0, 6.0, ((1, 8), (2, 96)), jnp.float32),
        "state_imag": gaussian(streams_of[14], (LAYERS, BATCH, G, P_SIZE), 1.0, 6.0, ((1, 8), (2, 96)), jnp.float32),
    }


PRECISION_LEVEL = lax.Precision.HIGHEST

def reference(tokens, gains, w_input, w_gating, w_output, decay_rate, frequency, log_step, in_real, in_imag, readout_real_matrix, readout_imag_matrix, skip_gain, state_real, state_imag):
    x = tokens
    outs_re = []
    outs_im = []
    batch = x.shape[0]
    for layer_params in range(LAYERS):
        xf = x.astype(jnp.float32)
        meansq = lax.optimization_barrier(jnp.mean(xf * xf, axis=1, keepdims=True))
        inverse = lax.rsqrt(meansq + 1e-06)
        scaled = (xf * gains[layer_params][None, :]).astype(jnp.bfloat16)
        drive = jnp.dot(scaled, w_input[layer_params], preferred_element_type=jnp.float32) * inverse
        gate = jnp.dot(scaled, w_gating[layer_params], preferred_element_type=jnp.float32) * inverse
        step = jnp.exp(log_step[layer_params])[:, None]
        lam_re = -decay_rate[layer_params]
        lam_im = frequency[layer_params]
        magnitude = jnp.exp(lam_re * step)
        angle = lam_im * step
        abar_re = magnitude * jnp.cos(angle)
        abar_im = magnitude * jnp.sin(angle)
        denom = lam_re * lam_re + lam_im * lam_im
        num_re = abar_re - 1.0
        zoh_re = (num_re * lam_re + abar_im * lam_im) / denom
        zoh_im = (abar_im * lam_re - num_re * lam_im) / denom
        bbar_re = zoh_re[..., None] * in_real[layer_params] - zoh_im[..., None] * in_imag[layer_params]
        bbar_im = zoh_re[..., None] * in_imag[layer_params] + zoh_im[..., None] * in_real[layer_params]
        grouped = drive.reshape(batch, G, GS)
        push_re = jnp.einsum('bgc,gpc->bgp', grouped, bbar_re, precision=PRECISION_LEVEL)
        push_im = jnp.einsum('bgc,gpc->bgp', grouped, bbar_im, precision=PRECISION_LEVEL)
        old_re = state_real[layer_params]
        old_im = state_imag[layer_params]
        updated_real = abar_re[None] * old_re - abar_im[None] * old_im + push_re
        updated_imag = abar_re[None] * old_im + abar_im[None] * old_re + push_im
        readout_output = jnp.einsum('zju,jiu->zji', updated_real, readout_real_matrix[layer_params], precision=PRECISION_LEVEL) - jnp.einsum('zju,jiu->zji', updated_imag, readout_imag_matrix[layer_params], precision=PRECISION_LEVEL)
        readout_output = readout_output + skip_gain[layer_params].reshape(G, GS)[None] * grouped
        gated = (jax.nn.gelu(readout_output.reshape(batch, G * GS)) * jax.nn.sigmoid(gate)).astype(jnp.bfloat16)
        branch = jnp.dot(gated, w_output[layer_params], preferred_element_type=jnp.float32)
        x = (xf + branch).astype(jnp.bfloat16)
        outs_re.append(updated_real)
        outs_im.append(updated_imag)
    return (x, jnp.stack(outs_re, axis=0), jnp.stack(outs_im, axis=0))
```

```python
import jax
import jax.numpy as jnp
from jax import lax
from jax.experimental import pallas as pl
from jax.experimental.pallas import tpu as pltpu
from jax.sharding import Mesh
from jax.sharding import PartitionSpec as P

MESH = pl.DeviceIdType.MESH
NZ, NY, NX = 12, 8, 4
LAYERS = 2
B = 24
F = 88
D = NZ * NY * F
C = 128
GROUPS, GS, PS = 8, 16, 64
K = NZ * F
KP = 1152
TILES = KP // 128
BF = jnp.bfloat16
F32 = jnp.float32


def far_first(n):
    return sorted(range(1, n), key=lambda h: -min(h, n - h))


def dot(a, b):
    return jnp.dot(a, b, preferred_element_type=F32)


def dot_t(a, b):
    return lax.dot_general(a, b, (((1,), (1,)), ((), ())), preferred_element_type=F32)


def parts(v):
    hi = v.astype(BF)
    return hi, (v - hi.astype(F32)).astype(BF)


def lanes_of(shape):
    return lax.broadcasted_iota(jnp.int32, shape, 1)


def body(
    tokens, gains, w_in, w_gate, w_out, decay, freq, log_step, in_re, in_im, ro_re, ro_im, skip,
    st_re, st_im,
    mixed, next_re, next_im,
    tok_v, gain_v, win_v, wg_v, wout_v, dec_v, frq_v, ls_v, ire_v, iim_v, rre_v, rim_v, skip_v,
    st_v, s_v, b_hi, b_lo, c_hi, c_lo, nxt_v,
    res_v, zbuf, ybuf, part_v, rsend, rrecv, zsend, zrecv, out_v,
    load_sem, wload_sem, store_sem, zs, zr, ys, yr, rys, ryr, rzs, rzr, xs, xr, cs, cr,
):
    z, y = lax.axis_index("z"), lax.axis_index("y")
    x, c = lax.axis_index("x"), lax.axis_index("c")

    def along(ax, h):
        n = {"z": NZ, "y": NY, "x": NX, "c": 2}[ax]
        return {ax: lax.rem({"z": z, "y": y, "x": x, "c": c}[ax] + h, n)}

    small = [
        (tokens, tok_v), (gains, gain_v), (decay, dec_v), (freq, frq_v), (log_step, ls_v),
        (in_re, ire_v), (in_im, iim_v), (ro_re, rre_v), (ro_im, rim_v), (skip, skip_v),
        (st_re, st_v.at[0]), (st_im, st_v.at[1]),
    ]
    loads = [pltpu.make_async_copy(a, b, load_sem.at[i]) for i, (a, b) in enumerate(small)]
    for cp in loads:
        cp.start()

    def wide(xx, cc):
        return 4 * cc, 3 * xx + 2 * cc

    def rows(zz):
        return pl.ds(pl.multiple_of(zz * F, 8), F)

    wloads = []
    for l in range(LAYERS):
        for m, (src, dst) in enumerate(((w_in, win_v), (w_gate, wg_v))):
            j0, za = wide(x, c)
            wloads.append(pltpu.make_async_copy(
                src.at[l, pl.ds(j0, 8)], dst.at[l, :, rows(za)], wload_sem.at[l, m, 0]))
            wloads.append(pltpu.make_async_copy(
                src.at[l, pl.ds(8 - 8 * c, 4)], dst.at[l, pl.ds(4 * c, 4), rows(3 * x + 1)],
                wload_sem.at[l, m, 1]))
    for cp in wloads:
        cp.start()
    oloads = [pltpu.make_async_copy(w_out.at[l], wout_v.at[l], wload_sem.at[l, 2, 0])
              for l in range(LAYERS)]
    for cp in oloads:
        cp.start()

    barrier = pltpu.get_barrier_semaphore()
    greet = [("z", h) for h in far_first(NZ)] + [("y", h) for h in far_first(NY)]
    greet += [("x", 1), ("x", NX - 1), ("c", 1)]
    for ax, h in greet:
        pl.semaphore_signal(barrier, inc=1, device_id=along(ax, h), device_id_type=MESH)

    for cp in loads:
        cp.wait()

    lane128 = lanes_of((B, 128))
    tp = z * NY + y

    def own_gains(l):
        t0 = (tp * F) // 128 - tp // (NZ * NY - 1)
        g2 = gain_v[pl.ds(l, 1), pl.ds(pl.multiple_of(t0 * 128, 128), 256)]
        g2 = jnp.broadcast_to(g2, (8, 256))
        g2 = pltpu.roll(g2, lax.rem(256 - (tp * F - t0 * 128), 256), 1)
        return g2[0:1, 0:128]

    def publish(l, xv):
        scaled = xv * own_gains(l)
        hi, lo = parts(jnp.sum(xv * xv, axis=1, keepdims=True))
        out = jnp.where(lane128 < F, scaled, 0.0)
        out = jnp.where(lane128 == F, hi.astype(F32), out)
        out = jnp.where(lane128 == F + 1, lo.astype(F32), out)
        zbuf[l, z] = out.astype(BF)

    def z_gather(l):
        return [pltpu.make_async_remote_copy(
            src_ref=zbuf.at[l, z], dst_ref=zbuf.at[l, z], send_sem=zs.at[l], recv_sem=zr.at[l],
            device_id=along("z", h), device_id_type=MESH) for h in far_first(NZ)]

    def z_gather_all(l):
        return pltpu.make_async_remote_copy(
            src_ref=zbuf.at[l, pl.ds(0, NZ - 1)], dst_ref=zbuf.at[l, pl.ds(0, NZ - 1)],
            send_sem=zs.at[l], recv_sem=zr.at[l], device_id=along("z", 1), device_id_type=MESH)

    def compact(l):
        tiles = [jnp.zeros((B, 128), F32) for _ in range(TILES)]
        total = jnp.zeros((B, 128), F32)
        for k in range(NZ):
            v = zbuf[l, k].astype(F32)
            total = total + v
            t, s = divmod(k * F, 128)
            r = pltpu.roll(v, s, 1) if s else v
            tiles[t] = jnp.where((lane128 >= s) & (lane128 < s + F), r, tiles[t])
            if s + F > 128:
                tiles[t + 1] = jnp.where(lane128 < s + F - 128, r, tiles[t + 1])
        sq = jnp.sum(jnp.where((lane128 >= F) & (lane128 < F + 2), total, 0.0), axis=1, keepdims=True)
        hi, lo = parts(sq)
        last = tiles[TILES - 1]
        last = jnp.where(lane128 == 96, hi.astype(F32), last)
        tiles[TILES - 1] = jnp.where(lane128 == 97, lo.astype(F32), last)
        for t in range(TILES):
            ybuf[l, y, :, t * 128:(t + 1) * 128] = tiles[t].astype(BF)

    def y_gather(l):
        return [pltpu.make_async_remote_copy(
            src_ref=ybuf.at[l, y], dst_ref=ybuf.at[l, y], send_sem=ys.at[l], recv_sem=yr.at[l],
            device_id=along("y", h), device_id_type=MESH) for h in far_first(NY)]

    def y_gather_all(l):
        return pltpu.make_async_remote_copy(
            src_ref=ybuf.at[l, pl.ds(0, NY - 1)], dst_ref=ybuf.at[l, pl.ds(0, NY - 1)],
            send_sem=ys.at[l], recv_sem=yr.at[l], device_id=along("y", 1), device_id_type=MESH)

    mats = (win_v, wg_v)

    def rows_copies(l, m, owner_x, owner_c, peer, ss, rs):
        w = mats[m]
        _, za = wide(owner_x, owner_c)
        a = w.at[l, :, rows(za)]
        b = w.at[l, pl.ds(4 * owner_c, 4), rows(3 * owner_x + 1)]
        return [pltpu.make_async_remote_copy(src_ref=r, dst_ref=r, send_sem=ss, recv_sem=rs,
                                             device_id=peer, device_id_type=MESH) for r in (a, b)]

    def rows_wait(l, m, ss, rs):
        w = mats[m].at[l, 0, pl.ds(0, K)]
        return pltpu.make_async_remote_copy(src_ref=w, dst_ref=w, send_sem=ss, recv_sem=rs,
                                            device_id=along("c", 1), device_id_type=MESH)

    right, left = along("x", 1), along("x", NX - 1)
    mate = along("c", 1)
    xr_of = lambda h: lax.rem(x + h, NX)

    x_groups = {
        0: (0, 0, right), 1: (1, 0, left), 2: (1, 0, right), 3: (0, 0, left),
        4: (0, NX - 1, right), 5: (1, 1, left),
    }

    def x_start(l, ids):
        for i in ids:
            m, h, peer = x_groups[i]
            for cp in rows_copies(l, m, xr_of(h), c, peer, xs.at[l, i], xr.at[l, i]):
                cp.start()

    def x_wait_recv(l, ids):
        for i in ids:
            rows_wait(l, x_groups[i][0], xs.at[l, i], xr.at[l, i]).wait_recv()

    def c_start(l, ids):
        for i in ids:
            m, h = i % 2, (0, NX - 1, 1, 2)[i // 2]
            for cp in rows_copies(l, m, xr_of(h), c, mate, cs.at[l, i], cr.at[l, i]):
                cp.start()

    def c_wait_recv(l):
        for i in range(8):
            rows_wait(l, i % 2, cs.at[l, i], cr.at[l, i]).wait_recv()

    def state_prep(l):
        step = jnp.broadcast_to(ls_v[pl.ds(l, 1), :], (GROUPS, GROUPS))
        diag = lax.broadcasted_iota(jnp.int32, (GROUPS, GROUPS), 0) == lanes_of((GROUPS, GROUPS))
        step = jnp.exp(jnp.sum(jnp.where(diag, step, 0.0), axis=1, keepdims=True))
        lr, li = -dec_v[l], frq_v[l]
        mag, ang = jnp.exp(lr * step), li * step
        are, aim = mag * jnp.cos(ang), mag * jnp.sin(ang)
        den = lr * lr + li * li
        nre = are - 1.0
        zre, zim = (nre * lr + aim * li) / den, (aim * lr - nre * li) / den
        a1 = jnp.concatenate([are, are], axis=1)
        a2 = jnp.concatenate([-aim, aim], axis=1)
        spread = lambda v: jnp.broadcast_to(v[:, None, :], (GROUPS, GS, PS)).reshape(C, PS)
        zre, zim = spread(zre), spread(zim)
        ire, iim = ire_v[l], iim_v[l]
        bmat = jnp.concatenate([zre * ire - zim * iim, zre * iim + zim * ire], axis=1)
        cmat = jnp.concatenate([rre_v[l], -rim_v[l]], axis=1)
        group = lax.broadcasted_iota(jnp.int32, (C, 128), 0) // GS
        for g in range(GROUPS):
            at = pl.ds(g * 128, 128)
            b_hi[l, :, at], b_lo[l, :, at] = parts(jnp.where(group == g, bmat, 0.0))
            c_hi[l, :, at], c_lo[l, :, at] = parts(jnp.where(group == g, cmat, 0.0))
            h = jnp.concatenate([st_v[0, l, pl.ds(g, B, stride=GROUPS), :],
                                 st_v[1, l, pl.ds(g, B, stride=GROUPS), :]], axis=1)
            s_v[l, :, at] = a1[g:g + 1] * h + a2[g:g + 1] * pltpu.roll(h, PS, 1)

    def mixer(l):
        drive = jnp.zeros((B, C), F32)
        gate = jnp.zeros((B, C), F32)
        sq = jnp.zeros((B, 128), F32)
        for k in range(NY):
            a = ybuf[l, k]
            drive = drive + dot(a[:, :K], win_v[l, k])
            gate = gate + dot(a[:, :K], wg_v[l, k])
            sq = sq + a[:, KP - 128:].astype(F32)
        sq = jnp.sum(jnp.where((lane128 >= 96) & (lane128 < 98), sq, 0.0), axis=1, keepdims=True)
        inverse = lax.rsqrt(sq * (1.0 / D) + 1e-06)
        drive, gate = drive * inverse, gate * inverse
        uh, ul = parts(drive)
        bh, bl = b_hi[l], b_lo[l]
        h = s_v[l] + (dot(uh, bh) + (dot(uh, bl) + dot(ul, bh)))
        hh, hl = parts(h)
        ch, cl = c_hi[l], c_lo[l]
        out = dot_t(hh, ch) + (dot_t(hh, cl) + dot_t(hl, ch))
        out = out + skip_v[pl.ds(l, 1), :] * drive
        s_v[l] = h
        gelu = 0.5 * out * (1.0 + jnp.tanh(0.7978845608028654 * (out + 0.044715 * (out * out * out))))
        return (gelu * (1.0 / (1.0 + jnp.exp(-gate)))).astype(BF)

    def store_states(l):
        for g in range(GROUPS):
            h = s_v[l, :, pl.ds(g * 128, 128)]
            nxt_v[0, l, pl.ds(g, B, stride=GROUPS), :] = h[:, :PS]
            nxt_v[1, l, pl.ds(g, B, stride=GROUPS), :] = pltpu.roll(h, PS, 1)[:, :PS]

    def project(l, gated):
        part_v[...] = dot(gated, wout_v[l])
        for yy in range(NY):
            tiles = [jnp.zeros((B, 128), F32) for _ in range(TILES)]
            for k in range(NZ):
                lo = (k * NY + yy) * F
                done = 0
                while done < F:
                    st, so = divmod(lo + done, 128)
                    tt, to = divmod(k * F + done, 128)
                    n = min(F - done, 128 - so, 128 - to)
                    v = part_v[:, st * 128:(st + 1) * 128]
                    sh = (to - so) % 128
                    v = pltpu.roll(v, sh, 1) if sh else v
                    tiles[tt] = jnp.where((lane128 >= to) & (lane128 < to + n), v, tiles[tt])
                    done += n
            for t in range(TILES):
                rsend[l, yy, :, t * 128:(t + 1) * 128] = tiles[t].astype(BF)

    def y_scatter(l):
        out = []
        for h in far_first(NY):
            to = lax.rem(y + h, NY)
            out.append(pltpu.make_async_remote_copy(
                src_ref=rsend.at[l, to], dst_ref=rrecv.at[l, h - 1], send_sem=rys.at[l],
                recv_sem=ryr.at[l], device_id={"y": to}, device_id_type=MESH))
        return out

    def y_scatter_all(l):
        return pltpu.make_async_remote_copy(
            src_ref=rrecv.at[l], dst_ref=rrecv.at[l], send_sem=rys.at[l], recv_sem=ryr.at[l],
            device_id=along("y", 1), device_id_type=MESH)

    def y_sum(l):
        total = rsend[l, y].astype(F32)
        for h in range(NY - 1):
            total = total + rrecv[l, h].astype(F32)
        tiles = [total[:, t * 128:(t + 1) * 128] for t in range(TILES)]
        for k in range(NZ):
            t, s = divmod(k * F, 128)
            v = pltpu.roll(tiles[t], 128 - s, 1) if s else tiles[t]
            if s + F > 128:
                w = pltpu.roll(tiles[t + 1], 128 - s, 1)
                v = jnp.where(lane128 < 128 - s, v, w)
            zsend[l, k] = v.astype(BF)

    def z_scatter(l):
        out = []
        for h in far_first(NZ):
            to = lax.rem(z + h, NZ)
            out.append(pltpu.make_async_remote_copy(
                src_ref=zsend.at[l, to], dst_ref=zrecv.at[l, h - 1], send_sem=rzs.at[l],
                recv_sem=rzr.at[l], device_id={"z": to}, device_id_type=MESH))
        return out

    def z_scatter_all(l):
        return pltpu.make_async_remote_copy(
            src_ref=zrecv.at[l], dst_ref=zrecv.at[l], send_sem=rzs.at[l], recv_sem=rzr.at[l],
            device_id=along("z", 1), device_id_type=MESH)

    def z_sum(l):
        total = zsend[l, z].astype(F32)
        for h in range(NZ - 1):
            total = total + zrecv[l, h].astype(F32)
        return total

    res_v[...] = jnp.zeros((B, 128), F32)
    res_v[:, :F] = tok_v[...].astype(F32)
    publish(0, res_v[...])
    for cp in wloads + oloads:
        cp.wait()
    pl.semaphore_wait(barrier, len(greet))

    for l in range(LAYERS):
        for cp in z_gather(l):
            cp.start()
        if l == 0:
            x_start(0, (0, 1, 2, 3))
            c_start(0, (0, 1))
            state_prep(0)
        else:
            x_wait_recv(1, (4, 5))
            c_start(1, (6, 7))
        z_gather_all(l).wait_recv()
        compact(l)
        for cp in y_gather(l):
            cp.start()
        if l == 0:
            x_wait_recv(0, (0, 1))
            x_start(0, (4, 5))
            c_start(0, (2, 5))
            state_prep(1)
            x_wait_recv(0, (2, 3))
            c_start(0, (3, 4))
        y_gather_all(l).wait_recv()
        if l == 0:
            x_wait_recv(0, (4, 5))
            c_start(0, (6, 7))
            x_start(1, (0, 1, 2, 3))
            c_start(1, (0, 1))
        c_wait_recv(l)
        gated = mixer(l)
        project(l, gated)
        for cp in y_scatter(l):
            cp.start()
        store_states(l)
        if l == 0:
            x_wait_recv(1, (0, 1))
            x_start(1, (4, 5))
            c_start(1, (2, 5))
        else:
            outs = [pltpu.make_async_copy(nxt_v.at[i], (next_re, next_im)[i], store_sem.at[i])
                    for i in range(2)]
            for cp in outs:
                cp.start()
        y_scatter_all(l).wait_recv()
        y_sum(l)
        for cp in z_scatter(l):
            cp.start()
        if l == 0:
            x_wait_recv(1, (2, 3))
            c_start(1, (3, 4))
        z_scatter_all(l).wait_recv()
        new = jnp.where(lane128 < F, res_v[...] + z_sum(l), 0.0).astype(BF)
        if l + 1 < LAYERS:
            res_v[...] = new.astype(F32)
            publish(l + 1, new.astype(F32))
        else:
            out_v[...] = new[:, :F]
    cp = pltpu.make_async_copy(out_v, mixed, store_sem.at[2])
    cp.start()
    for l in range(LAYERS):
        z_gather_all(l).wait_send()
        y_gather_all(l).wait_send()
        y_scatter_all(l).wait_send()
        z_scatter_all(l).wait_send()
        for i in range(6):
            rows_wait(l, x_groups[i][0], xs.at[l, i], xr.at[l, i]).wait_send()
        for i in range(8):
            rows_wait(l, i % 2, cs.at[l, i], cr.at[l, i]).wait_send()
    for o in outs:
        o.wait()
    cp.wait()


def on_device(tokens, gains, w_in, w_gate, w_out, decay, freq, log_step, in_re, in_im, ro_re, ro_im,
              skip, st_re, st_im):
    blocks = lambda w: w.reshape(LAYERS, NZ, F, C)
    flat = lambda s: s.reshape(LAYERS, B * GROUPS, PS)
    cols = lambda m: m.transpose(0, 1, 3, 2).reshape(LAYERS, C, PS)
    wide = lambda m: m.reshape(LAYERS, C, PS)
    args = (tokens, gains, blocks(w_in), blocks(w_gate), w_out, decay, freq, log_step, cols(in_re),
            cols(in_im), wide(ro_re), wide(ro_im), skip, flat(st_re), flat(st_im))
    any_ = pl.BlockSpec(memory_space=pl.ANY)
    V = pltpu.VMEM
    sem = pltpu.SemaphoreType.DMA
    L = LAYERS
    scratch = [
        V((B, F), BF), V((L, D), F32),
        V((L, NY, K, C), BF), V((L, NY, K, C), BF), V((L, C, D), BF),
        V((L, GROUPS, PS), F32), V((L, GROUPS, PS), F32), V((L, GROUPS), F32),
        V((L, C, PS), F32), V((L, C, PS), F32), V((L, C, PS), F32), V((L, C, PS), F32), V((L, C), F32),
        V((2, L, B * GROUPS, PS), F32), V((L, B, GROUPS * 128), F32),
        V((L, C, GROUPS * 128), BF), V((L, C, GROUPS * 128), BF),
        V((L, C, GROUPS * 128), BF), V((L, C, GROUPS * 128), BF),
        V((2, L, B * GROUPS, PS), F32),
        V((B, 128), F32), V((L, NZ, B, 128), BF), V((L, NY, B, KP), BF), V((B, D), F32),
        V((L, NY, B, KP), BF), V((L, NY - 1, B, KP), BF),
        V((L, NZ, B, 128), BF), V((L, NZ - 1, B, 128), BF), V((B, F), BF),
        sem((12,)), sem((L, 3, 2)), sem((3,)),
        sem((L,)), sem((L,)), sem((L,)), sem((L,)), sem((L,)), sem((L,)), sem((L,)), sem((L,)),
        sem((L, 6)), sem((L, 6)), sem((L, 8)), sem((L, 8)),
    ]
    mixed, nre, nim = pl.pallas_call(
        body,
        name="decode",
        out_shape=(jax.ShapeDtypeStruct((B, F), BF),
                   jax.ShapeDtypeStruct((L, B * GROUPS, PS), F32),
                   jax.ShapeDtypeStruct((L, B * GROUPS, PS), F32)),
        in_specs=[any_] * len(args),
        out_specs=(any_,) * 3,
        scratch_shapes=scratch,
        compiler_params=pltpu.CompilerParams(collective_id=0, has_side_effects=True,
                                             vmem_limit_bytes=56 * 2**20),
    )(*args)
    shape = (L, B, GROUPS, PS)
    return mixed, nre.reshape(shape), nim.reshape(shape)


def solution(mesh):
    torus = Mesh(mesh.devices.reshape(NZ, NY, NX, 2), ("z", "y", "x", "c"))
    tp, dp = ("z", "y"), ("x", "c")
    return jax.shard_map(
        on_device,
        mesh=torus,
        in_specs=(
            P(dp, tp), P(), P(None, dp, tp), P(None, dp, tp), P(None, tp, None), P(None, tp, None),
            P(None, tp, None), P(None, tp), P(None, tp, None, None), P(None, tp, None, None),
            P(None, tp, None, None), P(None, tp, None, None), P(None, tp),
            P(None, dp, tp, None), P(None, dp, tp, None),
        ),
        out_specs=(P(dp, tp), P(None, dp, tp, None), P(None, dp, tp, None)),
        check_vma=False,
    )
```

```python
import jax
import jax.numpy as jnp
from jax import lax
from jax.experimental import pallas as pl
from jax.experimental.pallas import tpu as pltpu
from jax.sharding import Mesh
from jax.sharding import PartitionSpec as P

MESH = pl.DeviceIdType.MESH
NZ, NY, NX = 12, 8, 4
LAYERS = 2
B = 24
F = 88
D = NZ * NY * F
C = 128
GROUPS, GS, PS = 8, 16, 64
K = NZ * F
KP = 1152
TILES = KP // 128
SEMS = 80
BF = jnp.bfloat16
F32 = jnp.float32


def far_first(n):
    return sorted(range(1, n), key=lambda h: -min(h, n - h))


def dot(a, b):
    return jnp.dot(a, b, preferred_element_type=F32)


def dot_t(a, b):
    return lax.dot_general(a, b, (((1,), (1,)), ((), ())), preferred_element_type=F32)


def parts(v):
    hi = v.astype(BF)
    return hi, (v - hi.astype(F32)).astype(BF)


def lanes_of(shape):
    return lax.broadcasted_iota(jnp.int32, shape, 1)


def body(
    tokens, gains, w_in, w_gate, w_out, decay, freq, log_step, in_re, in_im, ro_re, ro_im, skip,
    st_re, st_im,
    mixed, next_re, next_im,
    tok_v, gain_v, win_v, wg_v, stage_v, wout_v, wrow_v, wsend_v, wo_v,
    dec_v, frq_v, ls_v, ire_v, iim_v, rre_v, rim_v, skip_v,
    st_v, s_v, b_hi, b_lo, c_hi, c_lo,
    res_v, zbuf, ybuf, xl_v, part_v, rsend, rrecv, psend, precv, gbuf, zsend, zrecv,
    load_sem, wload_sem, ssem, rsem,
):
    z, y = lax.axis_index("z"), lax.axis_index("y")
    x, c = lax.axis_index("x"), lax.axis_index("c")
    scope = jax.named_scope

    def along(ax, h):
        n = {"z": NZ, "y": NY, "x": NX, "c": 2}[ax]
        return {ax: lax.rem({"z": z, "y": y, "x": x, "c": c}[ax] + h, n)}

    right, left, mate = along("x", 1), along("x", NX - 1), along("c", 1)

    barrier = pltpu.get_barrier_semaphore()
    greet = [("z", h) for h in far_first(NZ)] + [("y", h) for h in far_first(NY)]
    greet += [("x", 1), ("x", NX - 1), ("c", 1)]
    for ax, h in greet:
        pl.semaphore_signal(barrier, inc=1, device_id=along(ax, h), device_id_type=MESH)

    small = [
        (tokens, tok_v), (gains, gain_v), (decay, dec_v), (freq, frq_v), (log_step, ls_v),
        (in_re, ire_v), (in_im, iim_v), (ro_re, rre_v), (ro_im, rim_v), (skip, skip_v),
        (st_re, st_v.at[0]), (st_im, st_v.at[1]),
    ]
    loads = [pltpu.make_async_copy(a, b, load_sem.at[i]) for i, (a, b) in enumerate(small)]
    for cp in loads:
        cp.start()

    def rows(zz):
        return pl.ds(pl.multiple_of(zz * F, 8), F)

    mats = (win_v, wg_v)
    d16 = pl.ds(pl.multiple_of((2 * x + c) * 16, 16), 16)
    za, zb = 3 * x + 2 * c, 3 * x + 1
    has_b = (y // 4) == c

    def load(src, dst, k):
        cp = pltpu.make_async_copy(src, dst, wload_sem.at[k])
        cp.start()
        return cp

    wloads0 = []
    for m, src in enumerate((w_in, w_gate)):
        wloads0.append(load(src.at[0, pl.ds(4 * c, 8)], mats[m].at[0, :, rows(za)], 2 * m))
        wloads0.append(load(src.at[0, pl.ds(8 - 8 * c, 4)],
                            mats[m].at[0, pl.ds(4 * c, 4), rows(zb)], 2 * m + 1))
    oload = load(w_out.at[0], wout_v, 4)
    wloads1 = []
    for m, src in enumerate((w_in, w_gate)):
        wloads1.append(load(src.at[1], stage_v.at[m], 5 + m))
        wloads1.append(load(src.at[1, 4 * c + y], mats[m].at[1, y, rows(za)], 7 + m))
    rload = load(w_out.at[1, d16], wrow_v, 9)

    def own_b(m):
        src = (w_in, w_gate)[m]
        return pltpu.make_async_copy(
            src.at[1, 8 - 8 * c + lax.rem(y, 4)], mats[m].at[1, y, rows(zb)], wload_sem.at[10 + m])

    @pl.when(has_b)
    def _():
        own_b(0).start()
        own_b(1).start()

    names = {}

    def sem_of(key):
        return names.setdefault(key, len(names))

    def remote(src, dst, key, peer):
        k = sem_of(key)
        return pltpu.make_async_remote_copy(src_ref=src, dst_ref=dst, send_sem=ssem.at[k],
                                            recv_sem=rsem.at[k], device_id=peer, device_id_type=MESH)

    unsent = []

    def group(key, copies, size):
        for src, dst, peer in copies:
            remote(src, dst, key, peer).start()
        unsent.append((key, size))

    def arrived(key, size):
        remote(size, size, key, mate).wait_recv()

    with scope("small_loads"):
        for cp in loads:
            cp.wait()

    lane128 = lanes_of((B, 128))
    tp = z * NY + y

    def own_gains(l):
        t0 = (tp * F) // 128 - tp // (NZ * NY - 1)
        g2 = gain_v[pl.ds(l, 1), pl.ds(pl.multiple_of(t0 * 128, 128), 256)]
        g2 = jnp.broadcast_to(g2, (8, 256))
        g2 = pltpu.roll(g2, lax.rem(256 - (tp * F - t0 * 128), 256), 1)
        return g2[0:1, 0:128]

    def publish(l, xv):
        scaled = xv * own_gains(l)
        hi, lo = parts(jnp.sum(xv * xv, axis=1, keepdims=True))
        out = jnp.where(lane128 < F, scaled, 0.0)
        out = jnp.where(lane128 == F, hi.astype(F32), out)
        out = jnp.where(lane128 == F + 1, lo.astype(F32), out)
        zbuf[l, z] = out.astype(BF)

    def gather(key, buf, ax, n, me):
        group(key, [(buf.at[me], buf.at[me], along(ax, h)) for h in far_first(n)],
              buf.at[pl.ds(0, n - 1)])

    def scatter(key, src, dst, ax, n, me):
        copies = []
        for h in far_first(n):
            to = lax.rem(me + h, n)
            copies.append((src.at[to], dst.at[h - 1], {ax: to}))
        group(key, copies, dst)

    def compact(l, write):
        tiles = [jnp.zeros((B, 128), F32) for _ in range(TILES)]
        total = jnp.zeros((B, 128), F32)
        for k in range(NZ):
            v = zbuf[l, k].astype(F32)
            total = total + v
            t, s = divmod(k * F, 128)
            r = pltpu.roll(v, s, 1) if s else v
            tiles[t] = jnp.where((lane128 >= s) & (lane128 < s + F), r, tiles[t])
            if s + F > 128:
                tiles[t + 1] = jnp.where(lane128 < s + F - 128, r, tiles[t + 1])
        sq = jnp.sum(jnp.where((lane128 >= F) & (lane128 < F + 2), total, 0.0), axis=1, keepdims=True)
        hi, lo = parts(sq)
        last = tiles[TILES - 1]
        last = jnp.where(lane128 == 96, hi.astype(F32), last)
        tiles[TILES - 1] = jnp.where(lane128 == 97, lo.astype(F32), last)
        for t in range(TILES):
            write(t, tiles[t].astype(BF))

    def ring0(key, m, owner_x, peer):
        w = mats[m]
        a = w.at[0, :, rows(3 * owner_x + 2 * c)]
        b = w.at[0, pl.ds(4 * c, 4), rows(3 * owner_x + 1)]
        group(key, [(a, a, peer), (b, b, peer)], w.at[0, 0, pl.ds(0, K)])

    def ring0_wait(key):
        arrived(key, win_v.at[0, 0, pl.ds(0, K)])

    def ring1(key, m, owner_x, peer):
        w = mats[m]
        a = w.at[1, :, rows(3 * owner_x + 2 * c)]
        group(key + "a", [(a, a, peer)], a)
        b = w.at[1, :, rows(3 * owner_x + 1)]

        @pl.when(has_b)
        def _():
            remote(b, b, key + "b", peer).start()

        part_sent.append((key + "b", b, has_b))

    part_sent = []
    blocks8 = win_v.at[1, :, pl.ds(0, F)]

    def ring1_wait(key):
        arrived(key + "a", blocks8)

        @pl.when(has_b)
        def _():
            arrived(key + "b", blocks8)

    def mate1_wait(key):
        arrived(key + "a", blocks8)

        @pl.when(jnp.logical_not(has_b))
        def _():
            arrived(key + "b", blocks8)

    def exchange1(m):
        key, w = f"e{m}", mats[m]
        dst = w.at[1, y, rows(za)]
        copies = []
        for h in far_first(NY):
            to = lax.rem(y + h, NY)
            copies.append((stage_v.at[m, 4 * c + to], dst, {"y": to}))
        group(key + "a", copies, w.at[1, pl.ds(0, NY - 1), pl.ds(0, F)])
        dst_b = w.at[1, y, rows(zb)]
        for k in range(4):
            to = 4 * c + k

            @pl.when(to != y)
            def _():
                remote(stage_v.at[m, 8 - 8 * c + k], dst_b, key + "b", {"y": to}).start()

        part_sent.append((key + "b", w.at[1, pl.ds(0, 3), pl.ds(0, F)], has_b))
        part_sent.append((key + "b", w.at[1, pl.ds(0, 4), pl.ds(0, F)], jnp.logical_not(has_b)))

    def exchange1_wait(m):
        key, w = f"e{m}", mats[m]
        arrived(key + "a", w.at[1, pl.ds(0, NY - 1), pl.ds(0, F)])

        @pl.when(has_b)
        def _():
            arrived(key + "b", w.at[1, pl.ds(0, NY - 1), pl.ds(0, F)])

    x_of = lambda h: lax.rem(x + h, NX)
    names_of = ("in", "gate")

    def wo_rows(h, cc):
        return pl.ds(pl.multiple_of((2 * x_of(h) + cc) * 16, 16), 16)

    def relayout_out():
        lane16 = lanes_of((16, 128))
        for yy in range(NY):
            tiles = [jnp.zeros((16, 128), F32) for _ in range(TILES)]
            by_y(lambda st: wrow_v[:, st * 128:(st + 1) * 128].astype(F32), yy, tiles, lane16)
            for t in range(TILES):
                wsend_v[yy, :, t * 128:(t + 1) * 128] = tiles[t].astype(BF)
        wo_v[y, d16] = wsend_v[y]

    def by_y(tile_of, yy, tiles, lane):
        for k in range(NZ):
            lo, done = (k * NY + yy) * F, 0
            while done < F:
                st, so = divmod(lo + done, 128)
                tt, to = divmod(k * F + done, 128)
                n = min(F - done, 128 - so, 128 - to)
                v, sh = tile_of(st), (to - so) % 128
                v = pltpu.roll(v, sh, 1) if sh else v
                tiles[tt] = jnp.where((lane >= to) & (lane < to + n), v, tiles[tt])
                done += n

    def state_prep(l):
        step = jnp.broadcast_to(ls_v[pl.ds(l, 1), :], (GROUPS, GROUPS))
        diag = lax.broadcasted_iota(jnp.int32, (GROUPS, GROUPS), 0) == lanes_of((GROUPS, GROUPS))
        step = jnp.exp(jnp.sum(jnp.where(diag, step, 0.0), axis=1, keepdims=True))
        lr, li = -dec_v[l], frq_v[l]
        mag, ang = jnp.exp(lr * step), li * step
        are, aim = mag * jnp.cos(ang), mag * jnp.sin(ang)
        den = lr * lr + li * li
        nre = are - 1.0
        zre, zim = (nre * lr + aim * li) / den, (aim * lr - nre * li) / den
        a1 = jnp.concatenate([are, are], axis=1)
        a2 = jnp.concatenate([-aim, aim], axis=1)
        spread = lambda v: jnp.broadcast_to(v[:, None, :], (GROUPS, GS, PS)).reshape(C, PS)
        zre, zim = spread(zre), spread(zim)
        ire, iim = ire_v[l], iim_v[l]
        bmat = jnp.concatenate([zre * ire - zim * iim, zre * iim + zim * ire], axis=1)
        cmat = jnp.concatenate([rre_v[l], -rim_v[l]], axis=1)
        of = lax.broadcasted_iota(jnp.int32, (C, 128), 0) // GS
        for g in range(GROUPS):
            at = pl.ds(g * 128, 128)
            b_hi[l, :, at], b_lo[l, :, at] = parts(jnp.where(of == g, bmat, 0.0))
            c_hi[l, :, at], c_lo[l, :, at] = parts(jnp.where(of == g, cmat, 0.0))
            h = jnp.concatenate([st_v[0, l, pl.ds(g, B, stride=GROUPS), :],
                                 st_v[1, l, pl.ds(g, B, stride=GROUPS), :]], axis=1)
            s_v[l, :, at] = a1[g:g + 1] * h + a2[g:g + 1] * pltpu.roll(h, PS, 1)

    def mixer(l, drive, gate, sq):
        sq = jnp.sum(jnp.where((lane128 >= 96) & (lane128 < 98), sq, 0.0), axis=1, keepdims=True)
        inverse = lax.rsqrt(sq * (1.0 / D) + 1e-06)
        drive, gate = drive * inverse, gate * inverse
        uh, ul = parts(drive)
        bh, bl = b_hi[l], b_lo[l]
        h = s_v[l] + (dot(uh, bh) + (dot(uh, bl) + dot(ul, bh)))
        hh, hl = parts(h)
        ch, cl = c_hi[l], c_lo[l]
        out = dot_t(hh, ch) + (dot_t(hh, cl) + dot_t(hl, ch))
        out = out + skip_v[pl.ds(l, 1), :] * drive
        s_v[l] = h
        gelu = 0.5 * out * (1.0 + jnp.tanh(0.7978845608028654 * (out + 0.044715 * (out * out * out))))
        return (gelu * (1.0 / (1.0 + jnp.exp(-gate)))).astype(BF)

    def store_states(l):
        for g in range(GROUPS):
            h = s_v[l, :, pl.ds(g * 128, 128)]
            next_re[l, pl.ds(g, B, stride=GROUPS), :] = h[:, :PS]
            next_im[l, pl.ds(g, B, stride=GROUPS), :] = pltpu.roll(h, PS, 1)[:, :PS]

    def to_blocks(l, total):
        tiles = [total[:, t * 128:(t + 1) * 128] for t in range(TILES)]
        for k in range(NZ):
            t, s = divmod(k * F, 128)
            v = pltpu.roll(tiles[t], 128 - s, 1) if s else tiles[t]
            if s + F > 128:
                w = pltpu.roll(tiles[t + 1], 128 - s, 1)
                v = jnp.where(lane128 < 128 - s, v, w)
            zsend[l, k] = v.astype(BF)

    def z_reduce(l, meanwhile):
        with scope("zsc_start"):
            scatter(f"zs{l}", zsend.at[l], zrecv.at[l], "z", NZ, z)
        meanwhile()
        with scope("zsc_wait"):
            arrived(f"zs{l}", zrecv.at[l])
        with scope("z_sum"):
            total = zsend[l, z].astype(F32)
            for h in range(NZ - 1):
                total = total + zrecv[l, h].astype(F32)
            return jnp.where(lane128 < F, res_v[...] + total, 0.0).astype(BF)

    with scope("publish"):
        res_v[...] = jnp.zeros((B, 128), F32)
        res_v[:, :F] = tok_v[...].astype(F32)
        publish(0, res_v[...])
    with scope("barrier"):
        pl.semaphore_wait(barrier, len(greet))

    with scope("zag_start"):
        gather("zg0", zbuf.at[0], "z", NZ, z)
    with scope("loads"):
        for cp in wloads0:
            cp.wait()
    with scope("x_start0"):
        ring0("r_in", 0, x, right)
        ring0("l_gate", 1, x, left)
        ring0("r_gate", 1, x, right)
        ring0("l_in", 0, x, left)
        ring0("m_in", 0, x, mate)
        ring0("m_gate", 1, x, mate)
    with scope("e0_start"):
        for cp in wloads1:
            cp.wait()
        exchange1(0)
    with scope("prep0"):
        state_prep(0)
    with scope("zag_wait"):
        arrived("zg0", zbuf.at[0, pl.ds(0, NZ - 1)])
    with scope("compact"):
        def write0(t, v):
            ybuf[y, :, t * 128:(t + 1) * 128] = v
        compact(0, write0)
    with scope("yag_start"):
        gather("yg0", ybuf, "y", NY, y)
        exchange1(1)
    with scope("x01_0"):
        ring0_wait("r_in")
        ring0_wait("l_gate")
        ring0("rr_in", 0, x_of(NX - 1), right)
        ring0("ll_gate", 1, x_of(1), left)
        ring0("ml_in", 0, x_of(NX - 1), mate)
        ring0("mr_gate", 1, x_of(1), mate)
    with scope("prep1"):
        state_prep(1)
        rload.wait()
        relayout_out()
        oload.wait()

        @pl.when(has_b)
        def _():
            own_b(0).wait()
            own_b(1).wait()
    with scope("x23_0"):
        ring0_wait("r_gate")
        ring0_wait("l_in")
        ring0("ml_gate", 1, x_of(NX - 1), mate)
        ring0("mr_in", 0, x_of(1), mate)
    with scope("yag_wait"):
        arrived("yg0", ybuf.at[pl.ds(0, NY - 1)])
    with scope("x45_0"):
        ring0_wait("rr_in")
        ring0_wait("ll_gate")
    with scope("x_start1"):
        ring0("m2_in", 0, x_of(2), mate)
        ring0("m2_gate", 1, x_of(2), mate)
        exchange1_wait(0)
        ring1("R_in", 0, x, right)
        ring1("L_in", 0, x, left)
        ring1("M_in", 0, x, mate)
    with scope("c_wait"):
        for k in ("m_in", "m_gate", "ml_in", "mr_gate", "ml_gate", "mr_in", "m2_in", "m2_gate"):
            ring0_wait(k)
    with scope("mixer"):
        drive = jnp.zeros((B, C), F32)
        gate = jnp.zeros((B, C), F32)
        sq = jnp.zeros((B, 128), F32)
        for k in range(NY):
            a = ybuf[k]
            drive = drive + dot(a[:, :K], win_v[0, k])
            gate = gate + dot(a[:, :K], wg_v[0, k])
            sq = sq + a[:, KP - 128:].astype(F32)
        gated = mixer(0, drive, gate, sq)
    with scope("project"):
        part_v[...] = dot(gated, wout_v[...])
        for yy in range(NY):
            tiles = [jnp.zeros((B, 128), F32) for _ in range(TILES)]
            by_y(lambda st: part_v[:, st * 128:(st + 1) * 128], yy, tiles, lane128)
            for t in range(TILES):
                rsend[yy, :, t * 128:(t + 1) * 128] = tiles[t].astype(BF)
    with scope("ysc_start"):
        scatter("ys0", rsend, rrecv, "y", NY, y)
    with scope("store_states"):
        store_states(0)
    with scope("e1_wait"):
        exchange1_wait(1)
        ring1("R_gate", 1, x, right)
        ring1("L_gate", 1, x, left)
        ring1("M_gate", 1, x, mate)
    with scope("x_in1"):
        ring1_wait("R_in")
        ring1("RR_in", 0, x_of(NX - 1), right)
        ring1("Ml_in", 0, x_of(NX - 1), mate)
        ring1_wait("L_in")
        ring1("Mr_in", 0, x_of(1), mate)
    with scope("ysc_wait"):
        arrived("ys0", rrecv)
    with scope("y_sum"):
        total = rsend[y].astype(F32)
        for h in range(NY - 1):
            total = total + rrecv[h].astype(F32)
        to_blocks(0, total)

    def out_exchange():
        copies = []
        for h in far_first(NY):
            to = lax.rem(y + h, NY)
            copies.append((wsend_v.at[to], wo_v.at[y, d16], {"y": to}))
        group("oy", copies, wo_v.at[pl.ds(0, NY - 1), pl.ds(0, 16)])

    def after_z0():
        with scope("o_start"):
            out_exchange()
        with scope("x_gate1"):
            ring1_wait("L_gate")
            ring1("LL_gate", 1, x_of(1), left)
            ring1("Mr_gate", 1, x_of(1), mate)
            ring1_wait("R_gate")
            ring1("Ml_gate", 1, x_of(NX - 1), mate)

    new = z_reduce(0, after_z0)
    res_v[...] = new.astype(F32)
    publish(1, new.astype(F32))

    with scope("zag_start"):
        gather("zg1", zbuf.at[1], "z", NZ, z)
    with scope("x2_1"):
        ring1_wait("RR_in")
        ring1("M2_in", 0, x_of(2), mate)
        ring1_wait("LL_gate")
        ring1("M2_gate", 1, x_of(2), mate)

    def out_ring(key, h, peer, half):
        r = wo_v.at[half, wo_rows(h, c)]
        group(key, [(r, r, peer)], r)

    every, low, high = pl.ds(0, NY), pl.ds(0, NY // 2), pl.ds(NY // 2, NY // 2)
    with scope("o_x"):
        arrived("oy", wo_v.at[pl.ds(0, NY - 1), pl.ds(0, 16)])
        out_ring("or", 0, right, every)
        out_ring("ol", 0, left, every)
        out_ring("om", 0, mate, every)
    with scope("zag_wait"):
        arrived("zg1", zbuf.at[1, pl.ds(0, NZ - 1)])
    with scope("compact"):
        def write1(t, v):
            xl_v[:, t * 128:(t + 1) * 128] = v
        compact(1, write1)
    with scope("c_wait1"):
        for k in ("M_in", "M_gate", "Ml_in", "Mr_in", "Ml_gate", "Mr_gate", "M2_in", "M2_gate"):
            mate1_wait(k)
    with scope("partial"):
        a = xl_v[...]
        for k in range(NY):
            psend[k, :, 0:128] = dot(a[:, :K], win_v[1, k]).astype(BF)
            psend[k, :, 128:256] = dot(a[:, :K], wg_v[1, k]).astype(BF)
            psend[k, :, 256:384] = a[:, KP - 128:]
    with scope("ysc_start"):
        scatter("ys1", psend, precv, "y", NY, y)
    with scope("o_x2"):
        arrived("or", wo_v.at[every, pl.ds(0, 16)])
        out_ring("orr", NX - 1, right, low)
        out_ring("oml", NX - 1, mate, every)
        arrived("ol", wo_v.at[every, pl.ds(0, 16)])
        out_ring("oll", 1, left, high)
        out_ring("omr", 1, mate, every)
    with scope("ysc_wait"):
        arrived("ys1", precv)
    with scope("mixer"):
        total = psend[y].astype(F32)
        for h in range(NY - 1):
            total = total + precv[h].astype(F32)
        gated = mixer(1, total[:, :128], total[:, 128:256], total[:, 256:])
        gbuf[y] = gated
    with scope("gag_start"):
        gather("gg", gbuf, "y", NY, y)
    with scope("store_states"):
        store_states(1)
    with scope("o_x3"):
        arrived("orr", wo_v.at[low, pl.ds(0, 16)])
        arrived("oll", wo_v.at[high, pl.ds(0, 16)])
        out_ring("om2", 2, mate, every)
    with scope("gag_wait"):
        arrived("gg", gbuf.at[pl.ds(0, NY - 1)])
    with scope("o_wait"):
        for k in ("om", "oml", "omr", "om2"):
            arrived(k, wo_v.at[every, pl.ds(0, 16)])
    with scope("project"):
        total = dot(gbuf[0], wo_v[0])
        for k in range(1, NY):
            total = total + dot(gbuf[k], wo_v[k])
        to_blocks(1, total)
    new = z_reduce(1, lambda: None)
    mixed[...] = new[:, :F]
    with scope("finish"):
        for key, size in unsent:
            remote(size, size, key, mate).wait_send()
        for key, size, when in part_sent:
            pl.when(when)(lambda key=key, size=size: remote(size, size, key, mate).wait_send())
    assert len(names) <= SEMS, len(names)


def write_out(a, b, c, to_a, to_b, to_c, sems):
    copies = [pltpu.make_async_copy(v, o, sems.at[i])
              for i, (v, o) in enumerate(((b, to_b), (c, to_c), (a, to_a)))]
    for cp in copies:
        cp.start()
    for cp in copies:
        cp.wait()


def on_device(tokens, gains, w_in, w_gate, w_out, decay, freq, log_step, in_re, in_im, ro_re, ro_im,
              skip, st_re, st_im):
    blocks = lambda w: w.reshape(LAYERS, NZ, F, C)
    flat = lambda s: s.reshape(LAYERS, B * GROUPS, PS)
    cols = lambda m: m.transpose(0, 1, 3, 2).reshape(LAYERS, C, PS)
    wide = lambda m: m.reshape(LAYERS, C, PS)
    args = (tokens, gains, blocks(w_in), blocks(w_gate), w_out, decay, freq, log_step, cols(in_re),
            cols(in_im), wide(ro_re), wide(ro_im), skip, flat(st_re), flat(st_im))
    any_ = pl.BlockSpec(memory_space=pl.ANY)
    V = pltpu.VMEM
    sem = pltpu.SemaphoreType.DMA
    L = LAYERS
    scratch = [
        V((B, F), BF), V((L, D), F32),
        V((L, NY, K, C), BF), V((L, NY, K, C), BF), V((2, NZ, F, C), BF), V((C, D), BF),
        V((16, D), BF), V((NY, 16, KP), BF), V((NY, C, KP), BF),
        V((L, GROUPS, PS), F32), V((L, GROUPS, PS), F32), V((L, GROUPS), F32),
        V((L, C, PS), F32), V((L, C, PS), F32), V((L, C, PS), F32), V((L, C, PS), F32), V((L, C), F32),
        V((2, L, B * GROUPS, PS), F32), V((L, B, GROUPS * 128), F32),
        V((L, C, GROUPS * 128), BF), V((L, C, GROUPS * 128), BF),
        V((L, C, GROUPS * 128), BF), V((L, C, GROUPS * 128), BF),
        V((B, 128), F32), V((L, NZ, B, 128), BF), V((NY, B, KP), BF), V((B, KP), BF), V((B, D), F32),
        V((NY, B, KP), BF), V((NY - 1, B, KP), BF),
        V((NY, B, 384), BF), V((NY - 1, B, 384), BF), V((NY, B, C), BF),
        V((L, NZ, B, 128), BF), V((L, NZ - 1, B, 128), BF),
        sem((12,)), sem((12,)), sem((SEMS,)), sem((SEMS,)),
    ]
    shapes = (((B, F), BF), ((L, B * GROUPS, PS), F32), ((L, B * GROUPS, PS), F32))
    vmem = pl.BlockSpec(memory_space=pltpu.VMEM)
    held = pl.pallas_call(
        body,
        name="decode",
        out_shape=tuple(V(*sh) for sh in shapes),
        in_specs=[any_] * len(args),
        out_specs=(vmem,) * 3,
        scratch_shapes=scratch,
        compiler_params=pltpu.CompilerParams(collective_id=0, has_side_effects=True,
                                             vmem_limit_bytes=56 * 2**20),
    )(*args)
    mixed, nre, nim = pl.pallas_call(
        write_out,
        name="write_out",
        out_shape=tuple(jax.ShapeDtypeStruct(*sh) for sh in shapes),
        in_specs=[vmem] * 3,
        out_specs=(any_,) * 3,
        scratch_shapes=[sem((3,))],
    )(*(pltpu.with_memory_space_constraint(v, pltpu.VMEM) for v in held))
    shape = (L, B, GROUPS, PS)
    return mixed, nre.reshape(shape), nim.reshape(shape)


def solution(mesh):
    torus = Mesh(mesh.devices.reshape(NZ, NY, NX, 2), ("z", "y", "x", "c"))
    tp, dp = ("z", "y"), ("x", "c")
    return jax.shard_map(
        on_device,
        mesh=torus,
        in_specs=(
            P(dp, tp), P(), P(None, dp, tp), P(None, dp, tp), P(None, tp, None), P(None, tp, None),
            P(None, tp, None), P(None, tp), P(None, tp, None, None), P(None, tp, None, None),
            P(None, tp, None, None), P(None, tp, None, None), P(None, tp),
            P(None, dp, tp, None), P(None, dp, tp, None),
        ),
        out_specs=(P(dp, tp), P(None, dp, tp, None), P(None, dp, tp, None)),
        check_vma=False,
    )
```

```python
import jax
import jax.numpy as jnp
from jax import lax
from jax.experimental import pallas as pl
from jax.experimental.pallas import tpu as pltpu
from jax.sharding import Mesh
from jax.sharding import PartitionSpec as P

MESH = pl.DeviceIdType.MESH
NZ, NY, NX = 12, 8, 4
LAYERS = 2
B = 24
F = 88
D = NZ * NY * F
C = 128
GROUPS, GS, PS = 8, 16, 64
K = NZ * F
KP = 1152
TILES = KP // 128
SEMS = 76
RA, RB = 16, 8
TZ = 6
BF = jnp.bfloat16
F32 = jnp.float32


def far_first(n):
    return sorted(range(1, n), key=lambda h: -min(h, n - h))


def dot(a, b):
    return jnp.dot(a, b, preferred_element_type=F32)


def dot_t(a, b):
    return lax.dot_general(a, b, (((1,), (1,)), ((), ())), preferred_element_type=F32)


def parts(v):
    hi = v.astype(BF)
    return hi, (v - hi.astype(F32)).astype(BF)


def lanes_of(shape):
    return lax.broadcasted_iota(jnp.int32, shape, 1)


def body(
    tokens, gains, w_in, w_gate, w_out, decay, freq, log_step, in_re, in_im, ro_re, ro_im, skip,
    st_re, st_im,
    mixed, next_re, next_im,
    tok_v, gain_v, w_v, stage_v, wout_v, wrow_v, wsend_v, wo_v,
    dec_v, frq_v, ls_v, ire_v, iim_v, rre_v, rim_v, skip_v,
    st_v, s_v, b_hi, b_lo, c_hi, c_lo,
    res_v, zga, ygb, zgb, zbuf, ybuf, acc_v, part_v, rsend, rrecv, psend, precv, gbuf, zsend, zrecv,
    zsa, zra, zsb, zrb, ysb, yrb,
    load_sem, wload_sem, ssem, rsem, ready,
):
    z, y = lax.axis_index("z"), lax.axis_index("y")
    x, c = lax.axis_index("x"), lax.axis_index("c")
    scope = jax.named_scope

    def along(ax, h):
        n = {"z": NZ, "y": NY, "x": NX, "c": 2}[ax]
        return {ax: lax.rem({"z": z, "y": y, "x": x, "c": c}[ax] + h, n)}

    right, left, mate = along("x", 1), along("x", NX - 1), along("c", 1)

    barrier = pltpu.get_barrier_semaphore()
    greet = [("z", h) for h in (3, NZ - 3, 2, NZ - 2, 1, NZ - 1)]
    greet += [("y", h) for h in (2, NY - 2, 1, NY - 1)]
    greet += [("x", 1), ("x", NX - 1), ("c", 1)]
    for ax, h in greet:
        pl.semaphore_signal(barrier, inc=1, device_id=along(ax, h), device_id_type=MESH)

    small = [
        (tokens, tok_v), (gains, gain_v), (decay, dec_v), (freq, frq_v), (log_step, ls_v),
        (in_re, ire_v), (in_im, iim_v), (ro_re, rre_v), (ro_im, rim_v), (skip, skip_v),
        (st_re, st_v.at[0]), (st_im, st_v.at[1]),
    ]
    loads = [pltpu.make_async_copy(a, b, load_sem.at[i]) for i, (a, b) in enumerate(small)]
    for cp in loads:
        cp.start()

    def rows(zz):
        return pl.ds(pl.multiple_of(zz * F, 8), F)

    cols = (pl.ds(0, C), pl.ds(C, C))
    d16 = pl.ds(pl.multiple_of((2 * x + c) * 16, 16), 16)
    za, zb = 3 * x + 2 * c, 3 * x + 1
    has_b = (y // 4) == c

    def load(src, dst, k):
        cp = pltpu.make_async_copy(src, dst, wload_sem.at[k])
        cp.start()
        return cp

    wloads0 = []
    for m, src in enumerate((w_in, w_gate)):
        wloads0.append(load(src.at[0, pl.ds(4 * c, 8)], w_v.at[0, :, rows(za), cols[m]], 2 * m))
        wloads0.append(load(src.at[0, pl.ds(8 - 8 * c, 4)],
                            w_v.at[0, pl.ds(4 * c, 4), rows(zb), cols[m]], 2 * m + 1))
    oload = load(w_out.at[0], wout_v, 4)
    wloads1 = []
    for m, src in enumerate((w_in, w_gate)):
        wloads1.append(load(src.at[1], stage_v.at[m], 5 + m))
        wloads1.append(load(src.at[1, 4 * c + y], w_v.at[1, y, rows(za), cols[m]], 7 + m))
    rload = load(w_out.at[1, d16], wrow_v, 9)

    def own_b(m):
        src = (w_in, w_gate)[m]
        return pltpu.make_async_copy(
            src.at[1, 8 - 8 * c + lax.rem(y, 4)], w_v.at[1, y, rows(zb), cols[m]], wload_sem.at[10 + m])

    @pl.when(has_b)
    def _():
        own_b(0).start()
        own_b(1).start()

    names = {}

    def sem_of(key):
        return names.setdefault(key, len(names))

    def remote(src, dst, key, peer):
        k = sem_of(key)
        return pltpu.make_async_remote_copy(src_ref=src, dst_ref=dst, send_sem=ssem.at[0],
                                            recv_sem=rsem.at[k], device_id=peer, device_id_type=MESH)

    unsent = []

    def group(key, copies, size):
        for src, dst, peer in copies:
            remote(src, dst, key, peer).start()
        unsent.append((key, size))

    def arrived(key, size):
        remote(size, size, key, mate).wait_recv()

    with scope("small_loads"):
        for cp in loads:
            cp.wait()

    lane128 = lanes_of((B, 128))
    tp = z * NY + y

    def own_gains(l):
        t0 = (tp * F) // 128 - tp // (NZ * NY - 1)
        g2 = gain_v[pl.ds(l, 1), pl.ds(pl.multiple_of(t0 * 128, 128), 256)]
        g2 = jnp.broadcast_to(g2, (8, 256))
        g2 = pltpu.roll(g2, lax.rem(256 - (tp * F - t0 * 128), 256), 1)
        return g2[0:1, 0:128]

    def publish(l, xv):
        scaled = xv * own_gains(l)
        hi, lo = parts(jnp.sum(xv * xv, axis=1, keepdims=True))
        out = jnp.where(lane128 < F, scaled, 0.0)
        out = jnp.where(lane128 == F, hi.astype(F32), out)
        return jnp.where(lane128 == F + 1, lo.astype(F32), out).astype(BF)

    def gather(key, buf, ax, n, me, hs, apart=False):
        for h in hs:
            group(f"{key}_{h}" if apart else key, [(buf.at[me], buf.at[me], along(ax, h))], buf.at[0])

    def gathered(key, buf, n):
        arrived(key, buf.at[pl.ds(0, n - 1)])

    def scatter(key, src, dst, ax, n, me):
        copies = []
        for h in far_first(n):
            to = lax.rem(me + h, n)
            copies.append((src.at[to], dst.at[h - 1], {ax: to}))
        group(key, copies, dst)

    def compact(buf, n, tiles_n, write):
        shape = (buf.shape[1], 128)
        lane = lanes_of(shape)
        tiles = [jnp.zeros(shape, F32) for _ in range(tiles_n)]
        total = jnp.zeros(shape, F32)
        for k in range(n):
            v = buf[k].astype(F32)
            total = total + v
            t, s = divmod(k * F, 128)
            r = pltpu.roll(v, s, 1) if s else v
            tiles[t] = jnp.where((lane >= s) & (lane < s + F), r, tiles[t])
            if s + F > 128:
                tiles[t + 1] = jnp.where(lane < s + F - 128, r, tiles[t + 1])
        sq = jnp.sum(jnp.where((lane >= F) & (lane < F + 2), total, 0.0), axis=1, keepdims=True)
        hi, lo = parts(sq)
        last = jnp.where(lane == 96, hi.astype(F32), tiles[tiles_n - 1])
        tiles[tiles_n - 1] = jnp.where(lane == 97, lo.astype(F32), last)
        for t in range(tiles_n):
            write(t, tiles[t].astype(BF))

    def ring0(key, m, owner_x, peer, which=2):
        a = w_v.at[0, :, rows(3 * owner_x + 2 * c), cols[m]]
        b = w_v.at[0, pl.ds(4 * c, 4), rows(3 * owner_x + 1), cols[m]]
        if which == 2:
            group(key, [(a, a, peer), (b, b, peer)], w_v.at[0, 0, pl.ds(0, K), cols[0]])
        else:
            r = (a, b)[which]
            group(key, [(r, r, peer)], r)

    def ring0_wait(key, which=2):
        size = w_v.at[0, 0, pl.ds(0, K), cols[0]]
        if which < 2:
            size = w_v.at[0, pl.ds(0, (8, 4)[which]), pl.ds(0, F), cols[0]]
        arrived(key, size)

    def ring1(key, m, owner_x, peer):
        a = w_v.at[1, :, rows(3 * owner_x + 2 * c), cols[m]]
        group(key, [(a, a, peer)], a)
        b = w_v.at[1, :, rows(3 * owner_x + 1), cols[m]]

        @pl.when(has_b)
        def _():
            remote(b, b, key, peer).start()

        part_sent.append((key, b, has_b))

    part_sent = []
    no_b = jnp.logical_not(has_b)

    def arrived_either(key, whole):
        for when, n in ((whole, 2 * F), (jnp.logical_not(whole), F)):
            @pl.when(when)
            def _():
                arrived(key, w_v.at[1, :, pl.ds(0, n), cols[0]])

    def ring1_wait(key):
        arrived_either(key, has_b)

    def mate1_wait(key):
        arrived_either(key, no_b)

    def blocks(n):
        return w_v.at[1, pl.ds(0, n), pl.ds(0, F), cols[0]]

    def exchange1(m):
        key = f"e{m}"
        dst = w_v.at[1, y, rows(za), cols[m]]
        copies = []
        for h in far_first(NY):
            to = lax.rem(y + h, NY)
            copies.append((stage_v.at[m, 4 * c + to], dst, {"y": to}))
        group(key, copies, blocks(NY - 1))
        dst_b = w_v.at[1, y, rows(zb), cols[m]]
        for k in range(4):
            to = 4 * c + k

            @pl.when(to != y)
            def _():
                remote(stage_v.at[m, 8 - 8 * c + k], dst_b, key, {"y": to}).start()

        part_sent.append((key, blocks(3), has_b))
        part_sent.append((key, blocks(4), no_b))

    def exchange1_wait(m):
        for when, n in ((has_b, 2 * F), (no_b, F)):
            @pl.when(when)
            def _():
                arrived(f"e{m}", w_v.at[1, pl.ds(0, NY - 1), pl.ds(0, n), cols[0]])

    x_of = lambda h: lax.rem(x + h, NX)
    names_of = ("in", "gate")

    def wo_rows(h, cc):
        return pl.ds(pl.multiple_of((2 * x_of(h) + cc) * 16, 16), 16)

    def relayout_out():
        lane16 = lanes_of((16, 128))
        for yy in range(NY):
            tiles = [jnp.zeros((16, 128), F32) for _ in range(TILES)]
            by_y(lambda st: wrow_v[:, st * 128:(st + 1) * 128].astype(F32), yy, tiles, lane16)
            for t in range(TILES):
                wsend_v[yy, :, t * 128:(t + 1) * 128] = tiles[t].astype(BF)
        wo_v[y, d16] = wsend_v[y]

    def by_y(tile_of, yy, tiles, lane):
        runs(tiles, lane, lambda k: ((k * NY + yy) * F, tile_of))

    def runs(tiles, lane, source):
        for k in range(NZ):
            (lo, tile_of), done = source(k), 0
            while done < F:
                st, so = divmod(lo + done, 128)
                tt, to = divmod(k * F + done, 128)
                n = min(F - done, 128 - so, 128 - to)
                v, sh = tile_of(st), (to - so) % 128
                v = pltpu.roll(v, sh, 1) if sh else v
                tiles[tt] = jnp.where((lane >= to) & (lane < to + n), v, tiles[tt])
                done += n

    def state_prep(l):
        step = jnp.broadcast_to(ls_v[pl.ds(l, 1), :], (GROUPS, GROUPS))
        diag = lax.broadcasted_iota(jnp.int32, (GROUPS, GROUPS), 0) == lanes_of((GROUPS, GROUPS))
        step = jnp.exp(jnp.sum(jnp.where(diag, step, 0.0), axis=1, keepdims=True))
        lr, li = -dec_v[l], frq_v[l]
        mag, ang = jnp.exp(lr * step), li * step
        are, aim = mag * jnp.cos(ang), mag * jnp.sin(ang)
        den = lr * lr + li * li
        nre = are - 1.0
        zre, zim = (nre * lr + aim * li) / den, (aim * lr - nre * li) / den
        a1 = jnp.concatenate([are, are], axis=1)
        a2 = jnp.concatenate([-aim, aim], axis=1)
        spread = lambda v: jnp.broadcast_to(v[:, None, :], (GROUPS, GS, PS)).reshape(C, PS)
        zre, zim = spread(zre), spread(zim)
        ire, iim = ire_v[l], iim_v[l]
        bmat = jnp.concatenate([zre * ire - zim * iim, zre * iim + zim * ire], axis=1)
        cmat = jnp.concatenate([rre_v[l], -rim_v[l]], axis=1)
        of = lax.broadcasted_iota(jnp.int32, (C, 128), 0) // GS
        for g in range(GROUPS):
            at = pl.ds(g * 128, 128)
            b_hi[l, :, at], b_lo[l, :, at] = parts(jnp.where(of == g, bmat, 0.0))
            c_hi[l, :, at], c_lo[l, :, at] = parts(jnp.where(of == g, cmat, 0.0))
            h = jnp.concatenate([st_v[0, l, pl.ds(g, B, stride=GROUPS), :],
                                 st_v[1, l, pl.ds(g, B, stride=GROUPS), :]], axis=1)
            s_v[l, :, at] = a1[g:g + 1] * h + a2[g:g + 1] * pltpu.roll(h, PS, 1)

    def mixer(l, drive, gate, sq):
        sq = jnp.sum(jnp.where((lane128 >= 96) & (lane128 < 98), sq, 0.0), axis=1, keepdims=True)
        inverse = lax.rsqrt(sq * (1.0 / D) + 1e-06)
        drive, gate = drive * inverse, gate * inverse
        uh, ul = parts(drive)
        bh, bl = b_hi[l], b_lo[l]
        h = s_v[l] + (dot(uh, bh) + (dot(uh, bl) + dot(ul, bh)))
        hh, hl = parts(h)
        ch, cl = c_hi[l], c_lo[l]
        out = dot_t(hh, ch) + (dot_t(hh, cl) + dot_t(hl, ch))
        out = out + skip_v[pl.ds(l, 1), :] * drive
        s_v[l] = h
        gelu = 0.5 * out * (1.0 + jnp.tanh(0.7978845608028654 * (out + 0.044715 * (out * out * out))))
        return (gelu * (1.0 / (1.0 + jnp.exp(-gate)))).astype(BF)

    def store_states(l):
        for g in range(GROUPS):
            h = s_v[l, :, pl.ds(g * 128, 128)]
            next_re[l, pl.ds(g, B, stride=GROUPS), :] = h[:, :PS]
            next_im[l, pl.ds(g, B, stride=GROUPS), :] = pltpu.roll(h, PS, 1)[:, :PS]

    def to_blocks(into, total):
        tiles = [total[:, t * 128:(t + 1) * 128] for t in range(TILES)]
        lane = lanes_of(tiles[0].shape)
        for k in range(NZ):
            t, s = divmod(k * F, 128)
            v = pltpu.roll(tiles[t], 128 - s, 1) if s else tiles[t]
            if s + F > 128:
                w = pltpu.roll(tiles[t + 1], 128 - s, 1)
                v = jnp.where(lane < 128 - s, v, w)
            into[k] = v.astype(BF)

    with scope("publish"):
        res_v[...] = jnp.zeros((B, 128), F32)
        res_v[:, :F] = tok_v[...].astype(F32)
        out = publish(0, res_v[...])
        zga[z] = out[:RA]
        ygb[y] = out[RA:]
    with scope("barrier"):
        pl.semaphore_wait(barrier, len(greet))
        for ax, h, k in (("z", 3, 0), ("z", NZ - 3, 0), ("y", 2, 1), ("y", NY - 2, 1)):
            pl.semaphore_signal(ready.at[k], inc=1, device_id=along(ax, h), device_id_type=MESH)

    near_z, near_y = (3, NZ - 3, 2, NZ - 2, 1, NZ - 1), (2, NY - 2, 1, NY - 1)
    far_z = [h for h in far_first(NZ) if h not in near_z]
    far_y = [h for h in far_first(NY) if h not in near_y]
    with scope("loads"):
        for cp in wloads0:
            cp.wait()
    with scope("x_start0"):
        ring0("r_in", 0, x, right)
        ring0("l_gate", 1, x, left)
        ring0("r_gate", 1, x, right)
        ring0("l_in", 0, x, left)
        ring0("m_in", 0, x, mate)
        ring0("m_gate", 1, x, mate)
    with scope("ag_start"):
        gather("zga", zga, "z", NZ, z, near_z)
        gather("ygb", ygb, "y", NY, y, near_y)
        for cp in wloads1:
            cp.wait()
        pl.semaphore_wait(ready.at[1], 2)
        gather("ygb", ygb, "y", NY, y, far_y)
        pl.semaphore_wait(ready.at[0], 2)
        gather("zga", zga, "z", NZ, z, far_z)
    with scope("e0_start"):
        exchange1(0)
    with scope("prep0"):
        state_prep(0)
    with scope("ygb_wait"):
        gathered("ygb", ygb, NY)
    with scope("compact_b"):
        def write_b(t, v):
            zgb[z, :, t * 128:(t + 1) * 128] = v
        compact(ygb, NY, TZ, write_b)
    with scope("zgb_start"):
        gather("zgb", zgb, "z", NZ, z, far_first(NZ))
    with scope("zga_wait"):
        gathered("zga", zga, NZ)
    with scope("compact"):
        def write_a(t, v):
            ybuf[y, :RA, t * 128:(t + 1) * 128] = v
        compact(zga, NZ, TILES, write_a)
    with scope("yga_start"):
        a_rows = ybuf.at[:, pl.ds(0, RA)]
        gather("yga", a_rows, "y", NY, y, far_first(NY))
        exchange1(1)
    with scope("x01_0"):
        ring0_wait("r_in")
        ring0_wait("l_gate")
        for k in range(2):
            ring0(f"rr_in{k}", 0, x_of(NX - 1), right, k)
            ring0(f"ll_gate{k}", 1, x_of(1), left, k)
        ring0("ml_in", 0, x_of(NX - 1), mate)
        ring0("mr_gate", 1, x_of(1), mate)
    with scope("prep1"):
        state_prep(1)
        rload.wait()
        relayout_out()
        oload.wait()

        @pl.when(has_b)
        def _():
            own_b(0).wait()
            own_b(1).wait()
    with scope("x23_0"):
        ring0_wait("r_gate")
        ring0_wait("l_in")
        ring0("ml_gate", 1, x_of(NX - 1), mate)
        ring0("mr_in", 0, x_of(1), mate)
    with scope("zgb_wait"):
        gathered("zgb", zgb, NZ)
    with scope("regroup_b"):
        lane8 = lanes_of((RB, 128))
        sq_b = jnp.zeros((RB, 128), F32)
        for k in range(NZ):
            sq_b = sq_b + zgb[k, :, (TZ - 1) * 128:].astype(F32)
        for yy in range(NY):
            tiles = [jnp.zeros((RB, 128), F32) for _ in range(TILES)]
            runs(tiles, lane8, lambda k: (yy * F, lambda st: zgb[k, :, st * 128:(st + 1) * 128].astype(F32)))
            for t in range(TILES):
                ybuf[yy, RA:, t * 128:(t + 1) * 128] = tiles[t].astype(BF)
    with scope("yga_wait"):
        gathered("yga", a_rows, NY)
    with scope("x45_0"):
        for k in range(2):
            ring0_wait(f"rr_in{k}", k)
            ring0(f"m2_in{k}", 0, x_of(2), mate, k)
            ring0_wait(f"ll_gate{k}", k)
            ring0(f"m2_gate{k}", 1, x_of(2), mate, k)
    with scope("x_start1"):
        exchange1_wait(0)
        ring1("R_in", 0, x, right)
        ring1("L_in", 0, x, left)
        ring1("M_in", 0, x, mate)
    with scope("c_wait"):
        for k in ("m_in", "m_gate", "ml_in", "mr_gate", "ml_gate", "mr_in"):
            ring0_wait(k)
        for k in range(2):
            ring0_wait(f"m2_in{k}", k)
            ring0_wait(f"m2_gate{k}", k)
    with scope("mixer"):
        drive = jnp.zeros((B, C), F32)
        gate = jnp.zeros((B, C), F32)
        sq_a = jnp.zeros((RA, 128), F32)
        for k in range(NY):
            a = ybuf[k]
            drive = drive + dot(a[:, :K], w_v[0, k, :, :C])
            gate = gate + dot(a[:, :K], w_v[0, k, :, C:])
            sq_a = sq_a + a[:RA, KP - 128:].astype(F32)
        sq = jnp.concatenate([sq_a, sq_b], axis=0)
        gated = mixer(0, drive, gate, sq)
    with scope("project"):
        part_v[...] = dot(gated, wout_v[...])
        for k in range(NZ):
            for t in range(TZ):
                st, so = divmod(k * NY * F + t * 128, 128)
                v = part_v[RA:, st * 128:(st + 1) * 128]
                if so:
                    v = pltpu.roll(v, 64, 1)
                    if t < TZ - 1:
                        w = part_v[RA:, (st + 1) * 128:(st + 2) * 128]
                        v = jnp.where(lane8 < 64, v, pltpu.roll(w, 64, 1))
                zsb[k, :, t * 128:(t + 1) * 128] = v.astype(BF)
    with scope("zb_start"):
        scatter("zb", zsb, zrb, "z", NZ, z)
    with scope("project_a"):
        lane16 = lanes_of((RA, 128))
        for yy in range(NY):
            tiles = [jnp.zeros((RA, 128), F32) for _ in range(TILES)]
            by_y(lambda st: part_v[:RA, st * 128:(st + 1) * 128], yy, tiles, lane16)
            for t in range(TILES):
                rsend[yy, :, t * 128:(t + 1) * 128] = tiles[t].astype(BF)
    with scope("ysc_start"):
        scatter("ys0", rsend, rrecv, "y", NY, y)
    with scope("store_states"):
        store_states(0)
    with scope("e1_wait"):
        exchange1_wait(1)
        ring1("R_gate", 1, x, right)
        ring1("L_gate", 1, x, left)
        ring1("M_gate", 1, x, mate)
    with scope("x_in1"):
        ring1_wait("R_in")
        ring1("RR_in", 0, x_of(NX - 1), right)
        ring1("Ml_in", 0, x_of(NX - 1), mate)
        ring1_wait("L_in")
        ring1("Mr_in", 0, x_of(1), mate)
    with scope("zb_wait"):
        arrived("zb", zrb)
    with scope("zb_sum"):
        total = zsb[z].astype(F32)
        for h in range(NZ - 1):
            total = total + zrb[h].astype(F32)
        for yy in range(NY):
            t, so = divmod(yy * F, 128)
            v = total[:, t * 128:(t + 1) * 128]
            v = pltpu.roll(v, 128 - so, 1) if so else v
            if so + F > 128:
                w = pltpu.roll(total[:, (t + 1) * 128:(t + 2) * 128], 128 - so, 1)
                v = jnp.where(lane8 < 128 - so, v, w)
            ysb[yy] = v.astype(BF)
    with scope("yb_start"):
        scatter("yb", ysb, yrb, "y", NY, y)
    with scope("ysc_wait"):
        arrived("ys0", rrecv)
    with scope("y_sum"):
        total = rsend[y].astype(F32)
        for h in range(NY - 1):
            total = total + rrecv[h].astype(F32)
        to_blocks(zsa, total)

    def out_exchange():
        copies = []
        for h in far_first(NY):
            to = lax.rem(y + h, NY)
            copies.append((wsend_v.at[to], wo_v.at[y, d16], {"y": to}))
        group("oy", copies, wo_v.at[pl.ds(0, NY - 1), pl.ds(0, 16)])

    with scope("zsc_start"):
        scatter("zs0", zsa, zra, "z", NZ, z)
    with scope("o_start"):
        out_exchange()
    with scope("x_gate1"):
        ring1_wait("L_gate")
        ring1("LL_gate", 1, x_of(1), left)
        ring1("Mr_gate", 1, x_of(1), mate)
        ring1_wait("R_gate")
        ring1("Ml_gate", 1, x_of(NX - 1), mate)
    with scope("yb_wait"):
        arrived("yb", yrb)
    with scope("zsc_wait"):
        arrived("zs0", zra)
    with scope("z_sum"):
        total = zsa[z].astype(F32)
        for h in range(NZ - 1):
            total = total + zra[h].astype(F32)
        low_rows = ysb[y].astype(F32)
        for h in range(NY - 1):
            low_rows = low_rows + yrb[h].astype(F32)
        total = jnp.concatenate([total, low_rows], axis=0)
        new = jnp.where(lane128 < F, res_v[...] + total, 0.0).astype(BF)
    res_v[...] = new.astype(F32)
    zbuf[z] = publish(1, new.astype(F32))

    with scope("zag_start"):
        gather("zg1", zbuf, "z", NZ, z, far_first(NZ), True)
    with scope("x2_1"):
        ring1_wait("RR_in")
        ring1("M2_in", 0, x_of(2), mate)
        ring1_wait("LL_gate")
        ring1("M2_gate", 1, x_of(2), mate)

    def out_ring(key, h, peer, half):
        r = wo_v.at[half, wo_rows(h, c)]
        group(key, [(r, r, peer)], r)

    every, low, high = pl.ds(0, NY), pl.ds(0, NY // 2), pl.ds(NY // 2, NY // 2)
    with scope("o_x"):
        arrived("oy", wo_v.at[pl.ds(0, NY - 1), pl.ds(0, 16)])
        out_ring("or_l", 0, right, low)
        out_ring("ol_h", 0, left, high)
        out_ring("or_h", 0, right, high)
        out_ring("ol_l", 0, left, low)
        out_ring("om", 0, mate, every)
    with scope("c_wait1"):
        for k in ("M_in", "M_gate", "Ml_in", "Mr_in", "Ml_gate", "Mr_gate", "M2_in", "M2_gate"):
            mate1_wait(k)
    with scope("partial"):
        sq = jnp.zeros((B, 128), F32)
        for i, h in enumerate([0] + far_first(NZ)[::-1]):
            if h:
                arrived(f"zg1_{h}", zbuf.at[0])
            k = lax.rem(z + NZ - h, NZ)
            a = zbuf[k]
            sq = sq + a.astype(F32)
            for yy in range(NY):
                v = dot(a[:, :F], w_v[1, yy, rows(k), :])
                acc_v[yy] = acc_v[yy] + v if i else v
        sq = jnp.where((lane128 >= F) & (lane128 < F + 2), sq, 0.0)
        hi, lo = parts(jnp.sum(sq, axis=1, keepdims=True))
        sq = jnp.where(lane128 == 96, hi.astype(F32), jnp.where(lane128 == 97, lo.astype(F32), 0.0))
        for yy in range(NY):
            psend[yy, :, :2 * C] = acc_v[yy].astype(BF)
            psend[yy, :, 2 * C:] = sq.astype(BF)
    with scope("ysc_start"):
        scatter("ys1", psend, precv, "y", NY, y)
    with scope("o_x2"):
        arrived("or_l", wo_v.at[low, pl.ds(0, 16)])
        out_ring("orr", NX - 1, right, low)
        out_ring("oml_l", NX - 1, mate, low)
        arrived("ol_h", wo_v.at[high, pl.ds(0, 16)])
        out_ring("oll", 1, left, high)
        out_ring("omr_h", 1, mate, high)
    with scope("ysc_wait"):
        arrived("ys1", precv)
    with scope("mixer"):
        total = psend[y].astype(F32)
        for h in range(NY - 1):
            total = total + precv[h].astype(F32)
        gated = mixer(1, total[:, :128], total[:, 128:256], total[:, 256:])
        gbuf[y] = gated
    with scope("gag_start"):
        gather("gg", gbuf, "y", NY, y, far_first(NY), True)
    with scope("store_states"):
        store_states(1)
    with scope("o_x3"):
        arrived("or_h", wo_v.at[high, pl.ds(0, 16)])
        out_ring("oml_h", NX - 1, mate, high)
        arrived("ol_l", wo_v.at[low, pl.ds(0, 16)])
        out_ring("omr_l", 1, mate, low)
        arrived("orr", wo_v.at[low, pl.ds(0, 16)])
        out_ring("om2_l", 2, mate, low)
        arrived("oll", wo_v.at[high, pl.ds(0, 16)])
        out_ring("om2_h", 2, mate, high)
    with scope("o_wait"):
        arrived("om", wo_v.at[every, pl.ds(0, 16)])
        for k in ("oml", "omr", "om2"):
            arrived(k + "_l", wo_v.at[low, pl.ds(0, 16)])
            arrived(k + "_h", wo_v.at[high, pl.ds(0, 16)])
    with scope("project"):
        total = dot(gated, wo_v[y])
        for h in far_first(NY)[::-1]:
            arrived(f"gg_{h}", gbuf.at[0])
            k = lax.rem(y + NY - h, NY)
            total = total + dot(gbuf[k], wo_v[k])
        to_blocks(zsend, total)
    with scope("zsc_start"):
        scatter("zs1", zsend, zrecv, "z", NZ, z)
    with scope("zsc_wait"):
        arrived("zs1", zrecv)
    with scope("z_sum"):
        total = zsend[z].astype(F32)
        for h in range(NZ - 1):
            total = total + zrecv[h].astype(F32)
        mixed[...] = (res_v[...] + total).astype(BF)[:, :F]
    with scope("finish"):
        for key, size in unsent:
            remote(size, size, key, mate).wait_send()
        for key, size, when in part_sent:
            pl.when(when)(lambda key=key, size=size: remote(size, size, key, mate).wait_send())
    assert len(names) == SEMS, len(names)


def write_out(a, b, c, to_a, to_b, to_c, sems):
    copies = [pltpu.make_async_copy(v, o, sems.at[i])
              for i, (v, o) in enumerate(((b, to_b), (c, to_c), (a, to_a)))]
    for cp in copies:
        cp.start()
    for cp in copies:
        cp.wait()


def on_device(tokens, gains, w_in, w_gate, w_out, decay, freq, log_step, in_re, in_im, ro_re, ro_im,
              skip, st_re, st_im):
    blocks = lambda w: w.reshape(LAYERS, NZ, F, C)
    flat = lambda s: s.reshape(LAYERS, B * GROUPS, PS)
    cols = lambda m: m.transpose(0, 1, 3, 2).reshape(LAYERS, C, PS)
    wide = lambda m: m.reshape(LAYERS, C, PS)
    args = (tokens, gains, blocks(w_in), blocks(w_gate), w_out, decay, freq, log_step, cols(in_re),
            cols(in_im), wide(ro_re), wide(ro_im), skip, flat(st_re), flat(st_im))
    any_ = pl.BlockSpec(memory_space=pl.ANY)
    V = pltpu.VMEM
    sem = pltpu.SemaphoreType.DMA
    L = LAYERS
    scratch = [
        V((B, F), BF), V((L, D), F32),
        V((L, NY, K, 2 * C), BF), V((2, NZ, F, C), BF), V((C, D), BF),
        V((16, D), BF), V((NY, 16, KP), BF), V((NY, C, KP), BF),
        V((L, GROUPS, PS), F32), V((L, GROUPS, PS), F32), V((L, GROUPS), F32),
        V((L, C, PS), F32), V((L, C, PS), F32), V((L, C, PS), F32), V((L, C, PS), F32), V((L, C), F32),
        V((2, L, B * GROUPS, PS), F32), V((L, B, GROUPS * 128), F32),
        V((L, C, GROUPS * 128), BF), V((L, C, GROUPS * 128), BF),
        V((L, C, GROUPS * 128), BF), V((L, C, GROUPS * 128), BF),
        V((B, 128), F32), V((NZ, RA, 128), BF), V((NY, RB, 128), BF), V((NZ, RB, TZ * 128), BF),
        V((NZ, B, 128), BF), V((NY, B, KP), BF), V((NY, B, 2 * C), F32), V((B, D), F32),
        V((NY, RA, KP), BF), V((NY - 1, RA, KP), BF),
        V((NY, B, 384), BF), V((NY - 1, B, 384), BF), V((NY, B, C), BF),
        V((NZ, B, 128), BF), V((NZ - 1, B, 128), BF),
        V((NZ, RA, 128), BF), V((NZ - 1, RA, 128), BF),
        V((NZ, RB, TZ * 128), BF), V((NZ - 1, RB, TZ * 128), BF),
        V((NY, RB, 128), BF), V((NY - 1, RB, 128), BF),
        sem((12,)), sem((12,)), sem((1,)), sem((SEMS,)),
        pltpu.SemaphoreType.REGULAR((2,)),
    ]
    shapes = (((B, F), BF), ((L, B * GROUPS, PS), F32), ((L, B * GROUPS, PS), F32))
    vmem = pl.BlockSpec(memory_space=pltpu.VMEM)
    held = pl.pallas_call(
        body,
        name="decode",
        out_shape=tuple(V(*sh) for sh in shapes),
        in_specs=[any_] * len(args),
        out_specs=(vmem,) * 3,
        scratch_shapes=scratch,
        compiler_params=pltpu.CompilerParams(collective_id=0, has_side_effects=True,
                                             vmem_limit_bytes=56 * 2**20),
    )(*args)
    mixed, nre, nim = pl.pallas_call(
        write_out,
        name="write_out",
        out_shape=tuple(jax.ShapeDtypeStruct(*sh) for sh in shapes),
        in_specs=[vmem] * 3,
        out_specs=(any_,) * 3,
        scratch_shapes=[sem((3,))],
    )(*(pltpu.with_memory_space_constraint(v, pltpu.VMEM) for v in held))
    shape = (L, B, GROUPS, PS)
    return mixed, nre.reshape(shape), nim.reshape(shape)


def solution(mesh):
    torus = Mesh(mesh.devices.reshape(NZ, NY, NX, 2), ("z", "y", "x", "c"))
    tp, dp = ("z", "y"), ("x", "c")
    return jax.shard_map(
        on_device,
        mesh=torus,
        in_specs=(
            P(dp, tp), P(), P(None, dp, tp), P(None, dp, tp), P(None, tp, None), P(None, tp, None),
            P(None, tp, None), P(None, tp), P(None, tp, None, None), P(None, tp, None, None),
            P(None, tp, None, None), P(None, tp, None, None), P(None, tp),
            P(None, dp, tp, None), P(None, dp, tp, None),
        ),
        out_specs=(P(dp, tp), P(None, dp, tp, None), P(None, dp, tp, None)),
        check_vma=False,
    )
```
